32 devices in a mesh: ep: 4 (over y, x), tp: 8 (over z, core).
Axes of the slice: x: 2, y: 2, z: 4, core: 2. Of those that a mesh axis runs over, the one named last changes fastest.
Arguments:
- tokens: bfloat16 [256, 2048], P('ep'), may hold values from -7 to 7
- state: float32 [256, 32, 64, 64], P('ep', 'tp'), may hold values from -6 to 6
- routes: int32 [256, 2], P('ep'), may hold values from 0 to 3, all different within a row; in each aligned block of 64 rows (0 to 63, 64 to 127, ...) at most 48 rows name the same one
- route_logits: float32 [256, 2], P('ep'), may hold values from -4 to 4
- mix_gain: float32 [2048], replicated, may hold values from 0.1 to 1.9
- w_recept: bfloat16 [2048, 2048], P(None, 'tp')
- w_key: bfloat16 [2048, 2048], P(None, 'tp'), may hold values from -0.125 to 0.125
- w_value: bfloat16 [2048, 2048], P(None, 'tp'), may hold values from -0.125 to 0.125
- w_decay: bfloat16 [2048, 2048], P(None, 'tp'), may hold values from -0.125 to 0.125
- w_rate: bfloat16 [2048, 2048], P(None, 'tp'), may hold values from -0.125 to 0.125
- decay_base: float32 [2048], P('tp'), may hold values from -3 to 1
- rate_base: float32 [2048], P('tp'), may hold values from -3 to 3
- key_gain: float32 [2048], P('tp'), may hold values from 0.1 to 1.9
- group_gain: float32 [2048], P('tp'), may hold values from 0.1 to 1.9
- w_output: bfloat16 [2048, 2048], P('tp'), may hold values from -0.125 to 0.125
- ffn_gain: float32 [2048], replicated, may hold values from 0.1 to 1.9
- w_gate: bfloat16 [4, 2048, 7168], P('ep', None, 'tp'), may hold values from -0.125 to 0.125
- w_up: bfloat16 [4, 2048, 7168], P('ep', None, 'tp'), may hold values from -0.125 to 0.125
- w_down: bfloat16 [4, 7168, 2048], P('ep', 'tp'), may hold values from -0.0625 to 0.0625
Outputs:
- output: bfloat16 [256, 2048], P('ep', 'tp')
- new_state: float32 [256, 32, 64, 64], P('ep', 'tp')
The draws below stay inside these ranges and needn't reach their ends.
Inputs may be any that keep to these rules, and one draw needn't show every extreme that they name: `routes`: for each expert, the 64 tokens of one device group's rows name it in at most 48 of their rows; the 2 experts of a row differ.
All inputs are finite; a program needn't handle non-finite values.
Results may differ from the reference program's by a relative error of at most 0.0091.
Values may be sent and summed in bfloat16 or wider, within the bound.
A program may use at most 64 MiB of HBM per device.

```python
import math
from functools import partial
import jax
import jax.numpy as jnp
import numpy as np
from jax import lax

D = 2048
HEADS = 32
HEAD = 64
FF = 7168
TOPK = 2
SEQ_DEV = 64
SEQS = 256
EXPERTS = 4
CAP = 48
N_EP = 4


def draw_tokens(key, part):
    noise_key = jax.random.fold_in(key, 11)
    columns = jnp.exp(jnp.linspace(jnp.log(0.25), 0.0, D)).astype(jnp.float32)
    values = jnp.clip(jax.random.normal(noise_key, (SEQS, D), jnp.float32), -5.0, 5.0) * columns[None, :]
    return values.astype(jnp.bfloat16)


def draw_w_recept(key, part):
    entry_key = jax.random.fold_in(key, 21)
    scale_key = jax.random.fold_in(key, 22)
    head_scale = jnp.exp(jax.random.uniform(scale_key, (HEADS,), jnp.float32, jnp.log(0.001), jnp.log(0.01)))
    column_scale = jnp.repeat(head_scale, HEAD) * jnp.sqrt(64.0 / HEAD) / jnp.sqrt(1.0 * D)
    entries = jnp.clip(jax.random.normal(entry_key, (D, D), jnp.float32), -4.0, 4.0)
    values = entries * column_scale[None, :]
    return values.astype(jnp.bfloat16)


def steps_of(stream_key, extent, split, smallest, high):
    def one(position, blocks):
        heights = jax.random.uniform(jax.random.fold_in(jax.random.fold_in(stream_key, 6), position), (blocks,), jnp.float32, smallest / len(split), high / len(split))
        return jnp.repeat(jnp.exp(heights), extent[position] // blocks).reshape((-1,) + (1,) * (len(extent) - position - 1))

    gain = one(*split[0])
    for cut in split[1:]:
        gain = gain * one(*cut)
    return gain


def deal_out(own_key, own, number, rows, amount, top, bound, lean):
    ranking = jax.random.permutation(own_key, amount)
    crowded, usual = shares(amount, rows * top, bound, lean, True), shares(amount, rows * top, bound, lean, False)
    places = jnp.arange(amount)

    def named(sizes, rotation):
        used = int((sizes > 0).sum())
        fixed = max(1, used // 4)
        moved = fixed + (places - fixed + rotation * (used - fixed)) % max(1, amount - fixed)
        return jnp.zeros((amount,), jnp.int32).at[ranking[jnp.where(places < fixed, places, moved)]].set(jnp.asarray(sizes, jnp.int32))

    sizes = jnp.where(number % 4 == 0, named(crowded, number // 4), named(usual, number - number // 4 - 1))
    mixed = jax.random.permutation(jax.random.fold_in(own, 3), amount)
    source_of, taker = mixed[0:amount // 2 * 2:2], mixed[1:amount // 2 * 2:2]
    room = jnp.minimum(sizes[source_of] - 1, bound - sizes[taker]) // 2
    room = jnp.where((source_of == ranking[0]) | (taker == ranking[0]) | (sizes[taker] == 0), 0, jnp.maximum(room, 0))
    moved = jax.random.randint(jax.random.fold_in(own, 4), (amount // 2,), 0, 1 << 20) % (room + 1)
    sizes = sizes.at[source_of].add(-moved).at[taker].add(moved)
    labels = jnp.searchsorted(jnp.cumsum(sizes), jnp.arange(rows * top), side="right").astype(jnp.int32)
    table = labels.reshape(top, rows).T
    table = table[jax.random.permutation(jax.random.fold_in(own, 1), rows)]
    rotation = jax.random.randint(jax.random.fold_in(own, 2), (rows, 1), 0, top)
    return jnp.take_along_axis(table, (jnp.arange(top)[None, :] + rotation) % top, axis=1)


def shares(amount, total, bound, lean, full):
    portions = [(1 << 20) // math.isqrt(rank ** lean) + 1 for rank in range(1, amount + 1)]
    largest = bound if full else min(bound, max(-(-total // amount), total * portions[0] // sum(portions)))
    least = 1 if total - largest >= amount - 1 else 0
    given, rest = [largest] + [least] * (amount - 1), total - largest - least * (amount - 1)
    while rest > 0:
        movable = [i for i in range(1, amount) if given[i] < largest] or [i for i in range(1, amount) if given[i] < bound]
        pool, budget = sum([portions[i] for i in movable]), rest
        for i in movable:
            more = min(bound - given[i], max(1, budget * portions[i] // pool), rest)
            given[i] = given[i] + more
            rest = rest - more
    return np.array(given)


def noise(key, dims, width, limit, cuts=(), kind=jnp.bfloat16):
    drawn = width * jax.random.normal(key, dims, jnp.float32)
    if cuts:
        drawn = drawn * steps_of(key, dims, cuts, -0.22, 0.18)
    return jnp.clip(drawn, -limit, limit).astype(kind)


def setup_inputs(seed: int = 0) -> dict:
    key_of = jax.random.split(jax.random.key(seed), 20)
    tokens = draw_tokens(jax.random.fold_in(key_of[19], 71), 0)
    state = noise(key_of[1], (SEQS, HEADS, HEAD, HEAD), 1.0, 6.0, ((0, 4), (1, 8)), jnp.float32)
    routes_keys = jax.random.split(jax.random.fold_in(key_of[2], 1), SEQS // SEQ_DEV)
    routes_turns = jax.random.permutation(jax.random.fold_in(key_of[2], 3), SEQS // SEQ_DEV)
    routes = jax.vmap(lambda own, number: deal_out(jax.random.fold_in(key_of[2], 2), own, number, SEQ_DEV, EXPERTS, TOPK, CAP, 2))(routes_keys, routes_turns).reshape((SEQS, TOPK))
    route_logits = noise(key_of[3], (SEQS, TOPK), 1.5, 4.0, ((0, 4),), jnp.float32)
    mix_gain = jnp.clip(1.0 + 0.18 * jax.random.normal(key_of[4], (D,), jnp.float32), 0.1, 1.9)
    w_recept = draw_w_recept(jax.random.fold_in(key_of[19], 71), 0)
    w_key = noise(key_of[6], (D, D), D ** -0.5, 0.125, ((1, 8),))
    w_value = noise(key_of[7], (D, D), D ** -0.5, 0.125, ((1, 8),))
    w_decay = noise(key_of[8], (D, D), D ** -0.5, 0.125, ((1, 8),))
    w_rate = noise(key_of[9], (D, D), D ** -0.5, 0.125, ((1, 8),))
    decay_base = jnp.clip(-3.0 + 4.0 * jax.random.uniform(key_of[10], (D,), jnp.float32) ** steps_of(key_of[10], (D,), ((0, 8),), -0.2, 0.2), -3.0, 1.0)
    rate_base = noise(key_of[11], (D,), 1.0, 3.0, ((0, 8),), jnp.float32)
    key_gain = jnp.clip(1.0 + 0.18 * jax.random.normal(key_of[12], (D,), jnp.float32), 0.1, 1.9)
    group_gain = jnp.clip(1.0 + 0.18 * jax.random.normal(key_of[13], (D,), jnp.float32), 0.1, 1.9)
    w_output = noise(key_of[14], (D, D), D ** -0.5, 0.125, ((0, 8),))
    ffn_gain = jnp.clip(1.0 + 0.18 * jax.random.normal(key_of[15], (D,), jnp.float32), 0.1, 1.9)
    w_gate = noise(key_of[16], (EXPERTS, D, FF), D ** -0.5, 0.125, ((0, 4), (2, 8)))
    w_up = noise(key_of[17], (EXPERTS, D, FF), D ** -0.5, 0.125, ((0, 4), (2, 8)))
    w_down = noise(key_of[18], (EXPERTS, FF, D), FF ** -0.5, 0.0625, ((0, 4), (1, 8)))
    return {"tokens": tokens, "state": state, "routes": routes, "route_logits": route_logits, "mix_gain": mix_gain, "w_recept": w_recept, "w_key": w_key, "w_value": w_value, "w_decay": w_decay, "w_rate": w_rate, "decay_base": decay_base, "rate_base": rate_base, "key_gain": key_gain, "group_gain": group_gain, "w_output": w_output, "ffn_gain": ffn_gain, "w_gate": w_gate, "w_up": w_up, "w_down": w_down}


RMS_EPS = 1e-06
GROUP_EPS = 0.00064
UNIT_EPS = 6.4e-05
HIGHEST = lax.Precision.HIGHEST

def rounded(values):
    return lax.optimization_barrier(values.astype(jnp.bfloat16)).astype(jnp.float32)

def mix_heads(normed, state, w_recept, w_key, w_value, w_decay, w_rate, decay_base, rate_base, key_gain, group_gain):
    seq_rows = state.shape[0]
    head_count = state.shape[1]

    def project(weight):
        return rounded(jnp.dot(normed, weight, preferred_element_type=jnp.float32))

    def split_heads(values):
        return values.reshape(seq_rows, head_count, -1)
    recept = split_heads(project(w_recept))
    keys_now = split_heads(project(w_key))
    values_now = split_heads(project(w_value))
    decay_pre = project(w_decay) + decay_base
    decay_now = split_heads(jnp.exp(-jnp.exp(-jax.nn.softplus(-decay_pre) - 0.5)))
    rate_now = split_heads(jax.nn.sigmoid(project(w_rate) + rate_base))
    scaled = keys_now * key_gain.reshape(head_count, -1)[None]
    unit_key = scaled * lax.rsqrt(lax.optimization_barrier(jnp.sum(scaled * scaled, axis=2, keepdims=True)) + UNIT_EPS)
    removed = jnp.einsum('bhvk,bhk->bhv', state, unit_key, precision=HIGHEST)
    new_state = state * decay_now[:, :, None, :] - removed[:, :, :, None] * (unit_key * rate_now)[:, :, None, :] + values_now[:, :, :, None] * keys_now[:, :, None, :]
    readout = jnp.einsum('bhvk,bhk->bhv', new_state, recept, precision=HIGHEST)
    centred = readout - lax.optimization_barrier(jnp.mean(readout, axis=2, keepdims=True))
    spread = lax.optimization_barrier(jnp.mean(centred * centred, axis=2, keepdims=True))
    normed_read = centred * lax.rsqrt(spread + GROUP_EPS) * group_gain.reshape(head_count, -1)[None]
    return (normed_read.reshape(seq_rows, -1).astype(jnp.bfloat16), new_state)

def slot_numbers(route_rows, expert_count, capacity):
    flat_routes = route_rows.reshape(-1)
    one_hot = (flat_routes[:, None] == jnp.arange(expert_count, dtype=jnp.int32)[None, :]).astype(jnp.int32)
    earlier = jnp.cumsum(one_hot, axis=0) - one_hot
    placed = lax.optimization_barrier(jnp.sum(earlier * one_hot, axis=1)).astype(jnp.int32)
    return (flat_routes * capacity + placed).reshape(route_rows.shape)

def expert_rows(slot_rows, gate_weight, up_weight, down_weight):
    gate_act = jnp.dot(slot_rows, gate_weight, preferred_element_type=jnp.float32)
    upward = jnp.dot(slot_rows, up_weight, preferred_element_type=jnp.float32)
    hidden = (jax.nn.silu(gate_act) * upward).astype(jnp.bfloat16)
    return jnp.dot(hidden, down_weight, preferred_element_type=jnp.float32)

def reference(tokens, state, routes, route_logits, mix_gain, w_recept, w_key, w_value, w_decay, w_rate, decay_base, rate_base, key_gain, group_gain, w_output, ffn_gain, w_gate, w_up, w_down):
    values = tokens.astype(jnp.float32)
    normed = (values * lax.rsqrt(lax.optimization_barrier(jnp.mean(values * values, axis=1, keepdims=True)) + RMS_EPS) * mix_gain).astype(jnp.bfloat16)
    mixed_rows, new_state = mix_heads(normed, state, w_recept, w_key, w_value, w_decay, w_rate, decay_base, rate_base, key_gain, group_gain)
    residual = (values + jnp.dot(mixed_rows, w_output, preferred_element_type=jnp.float32)).astype(jnp.bfloat16)
    resid_vals = residual.astype(jnp.float32)
    ffn_in = (resid_vals * lax.rsqrt(lax.optimization_barrier(jnp.mean(resid_vals * resid_vals, axis=1, keepdims=True)) + RMS_EPS) * ffn_gain).astype(jnp.bfloat16)
    route_exp = jnp.exp(route_logits)
    route_weight = route_exp / lax.optimization_barrier(jnp.sum(route_exp, axis=1, keepdims=True))
    group_routes = routes.reshape(N_EP, SEQ_DEV, TOPK)
    slot_ids = jax.vmap(partial(slot_numbers, expert_count=EXPERTS, capacity=CAP))(group_routes)
    group_index = jnp.arange(N_EP, dtype=jnp.int32)
    local_token = jnp.broadcast_to(jnp.arange(SEQ_DEV, dtype=jnp.int32)[None, :, None], slot_ids.shape)
    global_token = local_token + (group_index * SEQ_DEV)[:, None, None]
    slot_flat = (slot_ids + (group_index * (EXPERTS * CAP))[:, None, None]).reshape(-1)
    owners_table = jnp.full((N_EP * EXPERTS * CAP,), SEQS, jnp.int32).at[slot_flat].set(global_token.reshape(-1))
    owners_table = owners_table.reshape(N_EP, EXPERTS, CAP).transpose(1, 0, 2).reshape(EXPERTS, N_EP * CAP)
    padded_in = jnp.concatenate([ffn_in, jnp.zeros((1, D), ffn_in.dtype)], axis=0)

    def one_expert(inputs):
        owners, gate_weight, up_weight, down_weight = inputs
        return expert_rows(padded_in[owners], gate_weight, up_weight, down_weight)
    outputs = lax.map(one_expert, (owners_table, w_gate, w_up, w_down)).reshape(EXPERTS, N_EP, CAP, D)
    place_in = (slot_ids - group_routes * CAP).astype(jnp.int32)
    picked = outputs[group_routes, group_index[:, None, None], place_in]
    moe_sum = lax.optimization_barrier(jnp.sum(picked * route_weight.reshape(N_EP, SEQ_DEV, TOPK)[..., None], axis=2)).reshape(SEQS, D)
    output = (resid_vals + moe_sum).astype(jnp.bfloat16)
    return (output, new_state)
```

```python
import jax
import jax.numpy as jnp
from jax import lax
from jax.experimental import pallas as pl
from jax.experimental.pallas import tpu as pltpu
from jax.sharding import PartitionSpec as P

MESH = pl.DeviceIdType.MESH

RMS_EPS = 1e-06
GROUP_EPS = 0.00064
UNIT_EPS = 6.4e-05


def mix_kernel(tokens, gain, w0, w1, w2, w3, w4, decay_base, rate_base, key_gain, group_gain, state, mixed, new_state,
               wbuf, work, unit_s, pull_s, scan_s, decay_s, key_s, value_s, removed_s, old_read, wsem, in_sem, out_sem):
    f32, bf16 = jnp.float32, jnp.bfloat16
    rows, heads, wide, _ = work.shape
    cols = heads * wide
    count = in_sem.shape[0]
    chunk = rows // count
    part = min(rows, 32)
    loads = [pltpu.make_async_copy(w, wbuf.at[i], wsem.at[i]) for i, w in enumerate((w1, w4, w3, w0, w2))]

    def fetch(b):
        spot = pl.ds(b * chunk, chunk)
        return pltpu.make_async_copy(state.at[spot], work.at[spot], in_sem.at[b])

    def put(b):
        spot = pl.ds(b * chunk, chunk)
        return pltpu.make_async_copy(work.at[spot], new_state.at[spot], out_sem.at[b])

    for load in loads:
        load.start()
    values = tokens[...].astype(f32)
    scale = lax.rsqrt(jnp.mean(values * values, axis=1, keepdims=True) + RMS_EPS)
    normed = (values * scale * gain[...]).astype(bf16)

    def project(i):
        loads[i].wait()
        for b in range(i * count // 5, (i + 1) * count // 5):
            fetch(b).start()
        return jnp.dot(normed, wbuf[i], preferred_element_type=f32).astype(bf16).astype(f32)

    def head(x, h):
        return x[:, h * wide : (h + 1) * wide]

    key = project(0)
    scaled = key * key_gain[...]
    squares = scaled * scaled
    rate = 1.0 / (1.0 + jnp.exp(-(project(1) + rate_base[...])))
    unit, pull = [], []
    for h in range(heads):
        length = jnp.sum(head(squares, h), axis=1, keepdims=True)
        unit.append(head(scaled, h) * lax.rsqrt(length + UNIT_EPS))
        pull.append(unit[h] * head(rate, h))
    open_part = 1.0 / (1.0 + jnp.exp(-(project(2) + decay_base[...])))
    decay = jnp.exp(-jnp.exp(-0.5) * open_part)
    recept = project(3)
    scan = decay * recept
    met = key * recept
    own, lost = [], []
    for h in range(heads):
        unit_s[h] = unit[h]
        scan_s[h] = head(scan, h)
        decay_s[h] = head(decay, h)
        key_s[h] = head(key, h)
        pull_s[h] = pull[h]
        own.append(jnp.sum(head(met, h), axis=1, keepdims=True))
        lost.append(jnp.sum(pull[h] * head(recept, h), axis=1, keepdims=True))
    value = project(4)
    value_s[...] = value

    per = max(1, 128 // wide)
    band = wide * per
    lane = lax.broadcasted_iota(jnp.int32, (8, band), 1) // wide
    sub = lax.broadcasted_iota(jnp.int32, (8, band), 0)

    def contract(b):
        spot = pl.ds(b * 8 if isinstance(b, int) else pl.multiple_of(b * 8, 8), 8)
        left = jnp.concatenate([ref[h, spot, :] for ref in (unit_s, scan_s) for h in range(heads)], axis=0).astype(bf16)
        sums = [jnp.zeros((8, band), f32)] * (2 * heads)
        for k in range(8):
            right = work[b * 8 + k].reshape(cols, wide).astype(bf16)
            got = lax.dot_general(left, right, (((1,), (1,)), ((), ())), preferred_element_type=f32)
            for g in range(2 * heads):
                low = (g % heads) // per * band
                sums[g] = jnp.where(sub == k, got[g * 8 : g * 8 + 8, low : low + band], sums[g])
        for ref, base in ((removed_s, 0), (old_read, heads)):
            for low in range(0, heads, per):
                piece = sums[base + low]
                for q in range(1, per):
                    piece = jnp.where(lane == q, sums[base + low + q], piece)
                ref[spot, low * wide : (low + per) * wide] = piece

    marks = lax.broadcasted_iota(jnp.int32, (wide, 4 * part), 1) % part

    def update(first, turned, right):
        for h in range(heads):
            left = turned[h * wide : (h + 1) * wide, :]
            stack = jnp.concatenate(
                [jnp.where(marks == (first + k) % part, left, 0.0).astype(bf16) for k in range(8)], axis=0
            )
            delta = jnp.dot(stack, right[h], preferred_element_type=f32)
            for k in range(8):
                s = first + k
                work[s, h] = work[s, h] * decay_s[h, s : s + 1, :] + delta[k * wide : (k + 1) * wide]

    per_chunk = chunk // 8
    for g in range(rows // part):
        span = slice(g * part, (g + 1) * part)
        for b in range(g * part // 8, (g + 1) * part // 8):
            if b % per_chunk == 0:
                fetch(b // per_chunk).wait()
            contract(b)
        removed = removed_s[span, :]
        high = removed.astype(bf16).astype(f32)
        turned = jnp.concatenate([high, removed - high, value_s[span, :], high], axis=0).T
        right = []
        for h in range(heads):
            p = pull_s[h, span, :]
            hi = p.astype(bf16).astype(f32)
            right.append(jnp.concatenate([-hi, -hi, key_s[h, span, :], hi - p], axis=0).astype(bf16))
        for b in range(g * part // 8, (g + 1) * part // 8):
            update(b * 8, turned, right)
            if (b + 1) % per_chunk == 0:
                put(b // per_chunk).start()
    removed = removed_s[...]
    old = old_read[...]
    for h in range(heads):
        lanes = slice(h * wide, (h + 1) * wide)
        out = old[:, lanes] - removed[:, lanes] * lost[h] + value[:, lanes] * own[h]
        centred = out - jnp.mean(out, axis=1, keepdims=True)
        spread = jnp.mean(centred * centred, axis=1, keepdims=True)
        mixed[:, lanes] = (centred * lax.rsqrt(spread + GROUP_EPS) * group_gain[:, lanes]).astype(bf16)
    for b in range(count):
        put(b).wait()


def mix_heads(tokens, state, mix_gain, projections, offsets):
    rows, width = tokens.shape
    _, heads, wide, _ = state.shape
    cols = heads * wide
    count = rows // 8
    f32 = jnp.float32
    vmem = pl.BlockSpec(memory_space=pltpu.VMEM)
    hbm = pl.BlockSpec(memory_space=pl.ANY)
    per_head = pltpu.VMEM((heads, rows, wide), f32)
    flat = pltpu.VMEM((rows, cols), f32)
    return pl.pallas_call(
        mix_kernel,
        out_shape=(
            jax.ShapeDtypeStruct((rows, cols), jnp.bfloat16),
            jax.ShapeDtypeStruct(state.shape, f32),
        ),
        in_specs=[vmem] * 2 + [hbm] * 5 + [vmem] * 4 + [hbm],
        out_specs=(vmem, hbm),
        scratch_shapes=[pltpu.VMEM((5, width, cols), jnp.bfloat16), pltpu.VMEM(state.shape, f32)]
        + [per_head] * 5
        + [flat] * 3
        + [pltpu.SemaphoreType.DMA((5,)), pltpu.SemaphoreType.DMA((count,)), pltpu.SemaphoreType.DMA((count,))],
        compiler_params=pltpu.CompilerParams(vmem_limit_bytes=67043328),
    )(tokens, mix_gain[None], *projections, *[x[None] for x in offsets], state)


def experts_kernel(
    mixed,
    tokens,
    routes,
    logits,
    gain,
    wo_hbm,
    wg_hbm,
    wu_hbm,
    wd_hbm,
    out,
    wo,
    wg,
    wu,
    wd,
    p1send,
    p1recv,
    z1send,
    z1recv,
    seg,
    wsend,
    wall,
    xn,
    hid,
    p4send,
    p4recv,
    e4send,
    e4recv,
    summed,
    kept,
    z4send,
    z4recv,
    load_sem,
    ws_sem,
    wr_sem,
    p1s_sem,
    p1r_sem,
    z1s_sem,
    z1r_sem,
    gz_sem,
    ge_sem,
    gp_sem,
    gr_sem,
    p4s_sem,
    p4r_sem,
    e4s_sem,
    e4r_sem,
    z4s_sem,
    z4r_sem,
):
    ep, tp = lax.axis_size("ep"), lax.axis_size("tp")
    nz = tp // 2
    e, t = lax.axis_index("ep"), lax.axis_index("tp")
    z, c = t // 2, lax.rem(t, 2)
    rows, width = tokens.shape
    cols = width // tp
    ff = wg.shape[1]
    f32, bf16 = jnp.float32, jnp.bfloat16
    loads = [
        pltpu.make_async_copy(a, b, load_sem.at[i])
        for i, (a, b) in enumerate(
            ((wo_hbm, wo), (wg_hbm.at[0], wg), (wu_hbm.at[0], wu), (wd_hbm.at[0], wd))
        )
    ]
    for load in loads:
        load.start()
    partner = (e, z * 2 + (1 - c))
    far = list(range(1, nz)) + [0]

    def zpeer(d):
        return lax.rem(z + d, nz)

    def epeer(d):
        return lax.rem(e + d, ep)

    def z_dev(d):
        return (e, zpeer(d) * 2 + c)

    def e_dev(d):
        return (epeer(d), t)

    def remote(src, dst, ssem, rsem, dev):
        return pltpu.make_async_remote_copy(
            src_ref=src, dst_ref=dst, send_sem=ssem, recv_sem=rsem, device_id=dev, device_id_type=MESH
        )

    barrier = pltpu.get_barrier_semaphore()
    peers = [partner] + [z_dev(d) for d in range(1, nz)] + [e_dev(d) for d in range(1, ep)]
    for peer in peers:
        pl.semaphore_signal(barrier, inc=1, device_id=peer, device_id_type=MESH)

    picked = jnp.exp(logits[...])
    picked = picked / jnp.sum(picked, axis=0, keepdims=True)
    names = routes[...]
    diagonal = lax.broadcasted_iota(jnp.int32, (rows, rows), 0) == lax.broadcasted_iota(
        jnp.int32, (rows, rows), 1
    )

    def weight_of(expert):
        line = jnp.sum(jnp.where(names == expert, picked, 0.0), axis=0, keepdims=True)
        column = jnp.sum(jnp.where(diagonal, line, 0.0), axis=1, keepdims=True)
        return jnp.broadcast_to(column, (rows, 128))

    wall[e] = weight_of(e)
    for d in range(1, ep):
        wsend[d] = weight_of(epeer(d))

    def block_of(ref, index):
        return ref[:, pl.ds(pl.multiple_of(index * cols, 128), cols)]

    loads[0].wait()
    pl.semaphore_wait(barrier, len(peers))
    started = []

    def start(copy):
        copy.start()
        started.append(copy)

    for d in far:
        zt = zpeer(d)
        part = jnp.dot(mixed[...], block_of(wo, zt * 2 + (1 - c)), preferred_element_type=f32)
        p1send[d] = part.astype(bf16)
        start(remote(p1send.at[d], p1recv.at[d], p1s_sem.at[d], p1r_sem.at[d], partner))
    for d in range(1, ep):
        start(remote(wsend.at[d], wall.at[e], ws_sem.at[d], wr_sem.at[d], e_dev(d)))
    for d in far:
        zt = zpeer(d)
        part = jnp.dot(mixed[...], block_of(wo, zt * 2 + c), preferred_element_type=f32)
        remote(p1send.at[d], p1recv.at[d], p1s_sem.at[d], p1r_sem.at[d], partner).wait_recv()
        part = part + p1recv[d].astype(f32)
        if d:
            z1send[d] = part.astype(bf16)
            start(remote(z1send.at[d], z1recv.at[d], z1s_sem.at[d], z1r_sem.at[d], z_dev(d)))
    part = part + block_of(tokens, t).astype(f32)
    for d in range(1, nz):
        remote(z1send.at[d], z1recv.at[d], z1s_sem.at[d], z1r_sem.at[d], z_dev(d)).wait_recv()
        part = part + z1recv[d].astype(f32)
    own = e * tp + t
    seg[own] = part.astype(bf16)

    def share(slot, ssem, dev):
        start(remote(seg.at[slot], seg.at[slot], ssem, gr_sem.at[slot], dev))

    def arrived(slot):
        remote(seg.at[slot], seg.at[slot], gz_sem.at[0], gr_sem.at[slot], partner).wait_recv()

    for d in range(1, nz):
        share(own, gz_sem.at[d], z_dev(d))
    for d in range(nz):
        slot = e * tp + zpeer(d) * 2 + c
        if d:
            arrived(slot)
        for k in range(1, ep):
            share(slot, ge_sem.at[d, k], e_dev(k))
        share(slot, gp_sem.at[0, d], partner)
    for d in range(nz):
        for k in range(1, ep):
            slot = epeer(k) * tp + zpeer(d) * 2 + c
            arrived(slot)
            share(slot, gp_sem.at[k, d], partner)
    for d in range(nz):
        for k in range(ep):
            arrived(epeer(k) * tp + zpeer(d) * 2 + (1 - c))
    for d in range(1, ep):
        remote(wsend.at[d], wall.at[epeer(d)], ws_sem.at[d], wr_sem.at[ep - d], e_dev(d)).wait_recv()

    def norm_group(g, carry):
        total = jnp.zeros((rows, cols), f32)
        for b in range(tp):
            x = seg[g * tp + b].astype(f32)
            total = total + x * x
        scale = lax.rsqrt(jnp.sum(total, axis=1, keepdims=True) / width + RMS_EPS)
        spot = pl.ds(pl.multiple_of(g * rows, rows), rows)
        for b in range(tp):
            lanes = slice(b * cols, (b + 1) * cols)
            xn[spot, lanes] = (seg[g * tp + b].astype(f32) * scale * gain[:, lanes]).astype(bf16)
        return carry

    lax.fori_loop(0, ep, norm_group, 0)
    for load in loads[1:]:
        load.wait()

    total_rows = ep * rows
    step = min(total_rows, 256)

    def hidden_rows(m, carry):
        spot = pl.ds(pl.multiple_of(m * step, step), step)
        for low in range(0, ff, 256):
            high = min(ff, low + 256)
            gate = jnp.dot(xn[spot, :], wg[:, low:high], preferred_element_type=f32)
            upward = jnp.dot(xn[spot, :], wu[:, low:high], preferred_element_type=f32)
            hid[spot, low:high] = (gate / (1.0 + jnp.exp(-gate)) * upward).astype(bf16)
        return carry

    lax.fori_loop(0, total_rows // step, hidden_rows, 0)

    def down(index):
        part = jnp.dot(hid[...], block_of(wd, index), preferred_element_type=f32)
        return part.reshape(ep, rows, cols) * wall[...][:, :, :1]

    for d in far:
        p4send[d] = down(zpeer(d) * 2 + (1 - c)).astype(bf16)
        start(remote(p4send.at[d], p4recv.at[d], p4s_sem.at[d], p4r_sem.at[d], partner))
    for d in far:
        part = down(zpeer(d) * 2 + c)
        remote(p4send.at[d], p4recv.at[d], p4s_sem.at[d], p4r_sem.at[d], partner).wait_recv()
        summed[...] = part + p4recv[d].astype(f32)
        e4send[d] = summed[...].astype(bf16)
        kept[d] = summed[e]
        for k in range(1, ep):
            start(
                remote(
                    e4send.at[d, epeer(k)], e4recv.at[d, k], e4s_sem.at[d, k], e4r_sem.at[d, k], e_dev(k)
                )
            )
    for d in far:
        part = kept[d]
        for k in range(1, ep):
            remote(
                e4send.at[d, epeer(k)], e4recv.at[d, k], e4s_sem.at[d, k], e4r_sem.at[d, k], e_dev(k)
            ).wait_recv()
            part = part + e4recv[d, k].astype(f32)
        if d:
            z4send[d] = part.astype(bf16)
            start(remote(z4send.at[d], z4recv.at[d], z4s_sem.at[d], z4r_sem.at[d], z_dev(d)))
    for d in range(1, nz):
        remote(z4send.at[d], z4recv.at[d], z4s_sem.at[d], z4r_sem.at[d], z_dev(d)).wait_recv()
        part = part + z4recv[d].astype(f32)
    out[...] = (seg[own].astype(f32) + part).astype(bf16)
    for copy in started:
        copy.wait_send()


def local(
    tokens,
    state,
    routes,
    route_logits,
    mix_gain,
    w_recept,
    w_key,
    w_value,
    w_decay,
    w_rate,
    decay_base,
    rate_base,
    key_gain,
    group_gain,
    w_output,
    ffn_gain,
    w_gate,
    w_up,
    w_down,
):
    seq_rows, full_width = tokens.shape
    mixed_rows, new_state = mix_heads(
        tokens,
        state,
        mix_gain,
        (w_recept, w_key, w_value, w_decay, w_rate),
        (decay_base, rate_base, key_gain, group_gain),
    )
    ep, tp = lax.axis_size("ep"), lax.axis_size("tp")
    nz = tp // 2
    cols = full_width // tp
    ff = w_gate.shape[2]
    heads_wide = w_output.shape[0]
    f32, bf16 = jnp.float32, jnp.bfloat16
    dma = pltpu.SemaphoreType.DMA
    vmem = pl.BlockSpec(memory_space=pltpu.VMEM)
    hbm = pl.BlockSpec(memory_space=pl.ANY)
    block = (nz, seq_rows, cols)
    output = pl.pallas_call(
        experts_kernel,
        out_shape=jax.ShapeDtypeStruct((seq_rows, cols), bf16),
        in_specs=[vmem] * 5 + [hbm] * 4,
        out_specs=vmem,
        scratch_shapes=[
            pltpu.VMEM((heads_wide, full_width), bf16),
            pltpu.VMEM((full_width, ff), bf16),
            pltpu.VMEM((full_width, ff), bf16),
            pltpu.VMEM((ff, full_width), bf16),
            pltpu.VMEM(block, bf16),
            pltpu.VMEM(block, bf16),
            pltpu.VMEM(block, bf16),
            pltpu.VMEM(block, bf16),
            pltpu.VMEM((ep * tp, seq_rows, cols), bf16),
            pltpu.VMEM((ep, seq_rows, 128), f32),
            pltpu.VMEM((ep, seq_rows, 128), f32),
            pltpu.VMEM((ep * seq_rows, full_width), bf16),
            pltpu.VMEM((ep * seq_rows, ff), bf16),
            pltpu.VMEM((nz, ep, seq_rows, cols), bf16),
            pltpu.VMEM((nz, ep, seq_rows, cols), bf16),
            pltpu.VMEM((nz, ep, seq_rows, cols), bf16),
            pltpu.VMEM((nz, ep, seq_rows, cols), bf16),
            pltpu.VMEM((ep, seq_rows, cols), f32),
            pltpu.VMEM(block, f32),
            pltpu.VMEM(block, bf16),
            pltpu.VMEM(block, bf16),
            dma((4,)),
            dma((ep,)),
            dma((ep,)),
            dma((nz,)),
            dma((nz,)),
            dma((nz,)),
            dma((nz,)),
            dma((nz,)),
            dma((nz, ep)),
            dma((ep, nz)),
            dma((ep * tp,)),
            dma((nz,)),
            dma((nz,)),
            dma((nz, ep)),
            dma((nz, ep)),
            dma((nz,)),
            dma((nz,)),
        ],
        compiler_params=pltpu.CompilerParams(
            collective_id=0, has_side_effects=True, vmem_limit_bytes=67043328
        ),
    )(mixed_rows, tokens, routes.T, route_logits.T, ffn_gain[None], w_output, w_gate, w_up, w_down)
    return (output, new_state)


def solution(mesh):
    placed = (
        P("ep", None),
        P("ep", "tp", None, None),
        P("ep", None),
        P("ep", None),
        P(),
        P(None, "tp"),
        P(None, "tp"),
        P(None, "tp"),
        P(None, "tp"),
        P(None, "tp"),
        P("tp"),
        P("tp"),
        P("tp"),
        P("tp"),
        P("tp", None),
        P(),
        P("ep", None, "tp"),
        P("ep", None, "tp"),
        P("ep", "tp", None),
    )
    return jax.shard_map(
        local,
        mesh=mesh,
        in_specs=placed,
        out_specs=(P("ep", "tp"), P("ep", "tp", None, None)),
        check_vma=False,
    )
```
